32 devices in a mesh: sp: 8 (over z, x), dp: 4 (over y, core).
Axes of the slice: x: 2, y: 2, z: 4, core: 2. Of those that a mesh axis runs over, the one named last changes fastest.
Arguments:
- lin_pre: bfloat16 [2048, 8192], P(None, ('dp', 'sp')), may hold values from -6 to 6
- gate_pre: bfloat16 [2048, 8192], P(None, ('dp', 'sp')), may hold values from -8 to 8
- w_depth: float32 [31, 2048], replicated, may hold values from -1 to 1
- ln_gain: float32 [2048], replicated, may hold values from 0.1 to 1.9
- ln_shift: float32 [2048], replicated, may hold values from -3 to 3
- w_out: bfloat16 [2048, 2048], P(None, 'dp'), may hold values from -0.125 to 0.125
Outputs:
- module_out: bfloat16 [8192, 2048], P(('dp', 'sp'))
The draws below stay inside these ranges and needn't reach their ends.
All inputs are finite; a program needn't handle non-finite values.
Results may differ from the reference program's by a relative error of at most 0.0064.
Values may be sent and summed in bfloat16 or wider, within the bound.
No kernel may reach another device: no remote copies, remote signals or barrier semaphores. Data moves between devices by JAX's collectives and lax.ppermute only.
A program may use at most 64 MiB of HBM per device.

```python
import jax
import jax.numpy as jnp
from jax import lax

D = 2048
KERNEL = 31
HALF = 15
LENGTH = 2048
TOKENS = 8192
N_DP = 4


def shard_levels(key, dims, split, low, top_value):
    gain = 1.0
    for axis_at, shards_of in split:
        steps = jax.random.uniform(jax.random.fold_in(jax.random.fold_in(key, 6), axis_at), (shards_of,), jnp.float32, low / len(split), top_value / len(split))
        gain = gain * jnp.repeat(jnp.exp(steps), dims[axis_at] // shards_of).reshape((-1,) + (1,) * (len(dims) - 1 - axis_at))
    return gain


def bell_draw(rng, dims, width, reach, pieces=(), dtype=jnp.bfloat16):
    values = width * jax.random.normal(rng, dims, jnp.float32)
    if pieces:
        values = values * shard_levels(rng, dims, pieces, -0.22, 0.18)
    return jnp.clip(values, -reach, reach).astype(dtype)


def setup_inputs(seed: int = 0) -> dict:
    seeds = jax.random.split(jax.random.key(seed), 7)
    lin_pre = bell_draw(seeds[0], (D, TOKENS), 1.0, 6.0, ((1, 32),))
    gate_pre = bell_draw(seeds[1], (D, TOKENS), 1.5, 8.0, ((1, 32),))
    w_depth = bell_draw(seeds[2], (KERNEL, D), KERNEL ** -0.5, 1.0, (), jnp.float32)
    ln_gain = jnp.clip(1.0 + 0.18 * jax.random.normal(seeds[3], (D,), jnp.float32), 0.1, 1.9)
    ln_shift = bell_draw(seeds[4], (D,), 0.5, 3.0, (), jnp.float32)
    w_out = bell_draw(seeds[5], (D, D), D ** -0.5, 0.125, ((1, 4),))
    return dict(lin_pre=lin_pre, gate_pre=gate_pre, w_depth=w_depth, ln_gain=ln_gain, ln_shift=ln_shift, w_out=w_out)


def one_sequence(glu_seq, w_depth, ln_gain, ln_shift, w_out):
    padded = jnp.pad(glu_seq.astype(jnp.float32), ((0, 0), (HALF, HALF)))
    running = jnp.zeros(glu_seq.shape, jnp.float32)
    for tap_index in range(KERNEL):
        running = running + w_depth[tap_index][:, None] * padded[:, tap_index:tap_index + LENGTH]
    mixed = running.astype(jnp.bfloat16)
    mixed_float = mixed.astype(jnp.float32)
    channel_mean = lax.optimization_barrier(jnp.mean(mixed_float, axis=0, keepdims=True))
    variance = lax.optimization_barrier(jnp.mean(jnp.square(mixed_float - channel_mean), axis=0, keepdims=True))
    normed = (mixed_float - channel_mean) * lax.rsqrt(variance + 1e-05)
    normed = normed * ln_gain[:, None] + ln_shift[:, None]
    activated = jax.nn.silu(normed).astype(jnp.bfloat16)
    projected = lax.dot_general(activated, w_out, (((0,), (0,)), ((), ())), preferred_element_type=jnp.float32)
    return projected.astype(jnp.bfloat16)

def reference(lin_pre, gate_pre, w_depth, ln_gain, ln_shift, w_out):
    glu = (lin_pre.astype(jnp.float32) * jax.nn.sigmoid(gate_pre.astype(jnp.float32))).astype(jnp.bfloat16)
    stacked = glu.reshape(D, N_DP, LENGTH).transpose(1, 0, 2)
    result = lax.map(lambda glu_seq: one_sequence(glu_seq, w_depth, ln_gain, ln_shift, w_out), stacked)
    return result.reshape(TOKENS, D)
```

```python
import functools

import jax
import jax.numpy as jnp
from jax import lax
from jax.experimental import pallas as pl
from jax.experimental.pallas import tpu as pltpu
from jax.sharding import PartitionSpec as P


LANES = 128
EDGE = 16
EPS = 1e-05


def params(semantics=None):
    return pltpu.CompilerParams(dimension_semantics=semantics, vmem_limit_bytes=48 << 20)


def cost(flops, nbytes):
    return pl.CostEstimate(flops=flops, transcendentals=0, bytes_accessed=nbytes)


def glu_body(lin_ref, gate_ref, out_ref, head_ref, tail_ref):
    gate = gate_ref[...].astype(jnp.float32)
    glu = (lin_ref[...].astype(jnp.float32) * jax.nn.sigmoid(gate)).T.astype(jnp.bfloat16)
    out_ref[...] = glu
    head_ref[...] = glu[:EDGE]
    tail_ref[...] = glu[glu.shape[0] - EDGE :]


def gated(lin_pre, gate_pre):
    channels, tokens = lin_pre.shape
    block = 256
    edge = pl.BlockSpec((EDGE, block), lambda i: (0, i))
    return pl.pallas_call(
        glu_body,
        grid=(channels // block,),
        in_specs=[pl.BlockSpec((block, tokens), lambda i: (i, 0))] * 2,
        out_specs=[pl.BlockSpec((tokens, block), lambda i: (0, i)), edge, edge],
        out_shape=[
            jax.ShapeDtypeStruct((tokens, channels), jnp.bfloat16),
            jax.ShapeDtypeStruct((EDGE, channels), jnp.bfloat16),
            jax.ShapeDtypeStruct((EDGE, channels), jnp.bfloat16),
        ],
        compiler_params=params(("arbitrary",)),
        cost_estimate=cost(20 * channels * tokens, 6 * channels * tokens),
        name="glu",
    )(lin_pre, gate_pre)


def conv_norm(cells, w_ref, gain_ref, shift_ref, mixed, start, tiles, store):
    blocks = cells.shape[0]
    span = 8 * tiles
    channels = blocks * LANES
    taps = w_ref.shape[0]

    def one_block(block, total):
        lanes = pl.ds(pl.multiple_of(block * LANES, LANES), LANES)
        running = [jnp.zeros((span, LANES), jnp.float32) for _ in range(2)]
        turn = 0
        lead = EDGE - (taps - 1) // 2
        for phase in range(8):
            window = cells[block, pl.ds(start - EDGE + phase, span + 8 * 3), :]
            for whole in range(4):
                tap = 8 * whole + phase - lead
                if 0 <= tap < taps:
                    weight = w_ref[pl.ds(tap, 1), lanes]
                    running[turn] = running[turn] + weight * window[8 * whole : 8 * whole + span]
                    turn = 1 - turn
        value = (running[0] + running[1]).astype(jnp.bfloat16).astype(jnp.float32)
        mixed[block, pl.ds(0, span), :] = value
        return total + value

    zeros = jnp.zeros((span, LANES), jnp.float32)
    total = lax.fori_loop(0, blocks, one_block, zeros)
    mean = jnp.broadcast_to(jnp.sum(total, axis=1, keepdims=True) / channels, (span, LANES))

    square = zeros
    for block in range(blocks):
        square = square + jnp.square(mixed[block, pl.ds(0, span), :] - mean)
    variance = jnp.sum(square, axis=1, keepdims=True) / channels
    scale = jnp.broadcast_to(lax.rsqrt(variance + EPS), (span, LANES))
    for block in range(blocks):
        lanes = pl.ds(block * LANES, LANES)
        normed = (mixed[block, pl.ds(0, span), :] - mean) * scale
        normed = normed * gain_ref[:, lanes] + shift_ref[:, lanes]
        store(lanes, (normed * jax.nn.sigmoid(normed)).astype(jnp.bfloat16))


def inner_body(tiles, glu_ref, w_ref, gain_ref, shift_ref, out_ref, cells, mixed):
    blocks = cells.shape[0]
    for block in range(blocks):
        cells[block] = glu_ref[:, pl.ds(block * LANES, LANES)].astype(jnp.float32)
    span = 8 * tiles

    def chunk(i, carry):
        start = pl.multiple_of(EDGE + i * span, 8)

        def store(lanes, value):
            out_ref[pl.ds(start, span), lanes] = value

        conv_norm(cells, w_ref, gain_ref, shift_ref, mixed, start, tiles, store)
        return carry

    lax.fori_loop(0, (glu_ref.shape[0] - 2 * EDGE) // span, chunk, 0)


def outer_body(before_ref, after_ref, glu_ref, w_ref, gain_ref, shift_ref, _, out_ref, cells, mixed):
    side = pl.program_id(0)
    blocks = cells.shape[0]
    for block in range(blocks):
        lanes = pl.ds(block * LANES, LANES)
        own = glu_ref[:, lanes].astype(jnp.float32)
        halo = jnp.where(side == 0, before_ref[:, lanes], after_ref[:, lanes]).astype(jnp.float32)
        cells[block, pl.ds(EDGE, 2 * EDGE), :] = jnp.where(side == 0, own, 0.0)
        cells[block, pl.ds(0, EDGE), :] = jnp.where(side == 0, halo, own[:EDGE])
        cells[block, pl.ds(EDGE, EDGE), :] = jnp.where(side == 0, own[:EDGE], own[EDGE:])
        cells[block, pl.ds(2 * EDGE, EDGE), :] = jnp.where(side == 0, own[EDGE:], halo)

    def store(lanes, value):
        out_ref[:, lanes] = value

    conv_norm(cells, w_ref, gain_ref, shift_ref, mixed, EDGE, EDGE // 8, store)


def activated_inner(glu, w_depth, gain, shift):
    tokens, channels = glu.shape
    inner = (tokens - 2 * EDGE) // 16
    tiles = 2 * max(n for n in range(1, 5) if inner % n == 0)
    blocks = channels // LANES
    return pl.pallas_call(
        functools.partial(inner_body, tiles),
        out_shape=jax.ShapeDtypeStruct((tokens, channels), jnp.bfloat16),
        scratch_shapes=[
            pltpu.VMEM((blocks, tokens, LANES), jnp.float32),
            pltpu.VMEM((blocks, 8 * tiles, LANES), jnp.float32),
        ],
        compiler_params=params(),
        cost_estimate=cost(80 * channels * tokens, 4 * channels * tokens),
        name="conv_inner",
    )(glu, w_depth, gain, shift)


def activated_outer(before, after, glu, w_depth, gain, shift, act):
    tokens, channels = glu.shape
    blocks = channels // LANES
    whole = pl.BlockSpec((EDGE, channels), lambda i: (0, 0))
    row = pl.BlockSpec((1, channels), lambda i: (0, 0))
    last = tokens // EDGE - 1
    return pl.pallas_call(
        outer_body,
        grid=(2,),
        in_specs=[
            whole,
            whole,
            pl.BlockSpec((2 * EDGE, channels), lambda i: (i * (tokens // (2 * EDGE) - 1), 0)),
            pl.BlockSpec(w_depth.shape, lambda i: (0, 0)),
            row,
            row,
            pl.BlockSpec(memory_space=pl.ANY),
        ],
        out_specs=pl.BlockSpec((EDGE, channels), lambda i: (i * last, 0)),
        out_shape=jax.ShapeDtypeStruct((tokens, channels), jnp.bfloat16),
        scratch_shapes=[
            pltpu.VMEM((blocks, 3 * EDGE, LANES), jnp.float32),
            pltpu.VMEM((blocks, EDGE, LANES), jnp.float32),
        ],
        input_output_aliases={6: 0},
        compiler_params=params(("arbitrary",)),
        cost_estimate=cost(80 * channels * 2 * EDGE, 8 * channels * EDGE),
        name="conv_outer",
    )(before, after, glu, w_depth, gain, shift, act)


def project_body(count, place_ref, act_ref, *refs):
    chunks, out_ref = refs[:count], refs[-1]
    rows = chunks[0].shape[0]
    total = None
    for i, chunk in enumerate(chunks):
        if count == 1:
            part = act_ref[...]
        else:
            part = act_ref[:, pl.ds(pl.multiple_of(place_ref[1 + i] * rows, LANES), rows)]
        term = jnp.dot(part, chunk[...], preferred_element_type=jnp.float32)
        total = term if total is None else total + term
    out_ref[...] = total.astype(jnp.bfloat16)


def project(act, chunks, units, shard, columns, out):
    tokens, channels = act.shape
    rows, width = chunks[0].shape
    block = min(width, 256)
    steps = width // block
    place = jnp.stack([jnp.asarray(v, jnp.int32) for v in (shard, *units)])
    in_specs = [pl.BlockSpec((tokens, channels), lambda i, place: (0, 0))]
    in_specs += [pl.BlockSpec((rows, block), lambda i, place: (0, i))] * len(chunks)
    operands = [act, *chunks]
    aliases = {}
    if out is not None:
        aliases = {len(operands) + 1: 0}
        in_specs.append(pl.BlockSpec(memory_space=pl.ANY))
        operands.append(out)
    return pl.pallas_call(
        functools.partial(project_body, len(chunks)),
        grid_spec=pltpu.PrefetchScalarGridSpec(
            num_scalar_prefetch=1,
            grid=(steps,),
            in_specs=in_specs,
            out_specs=pl.BlockSpec((tokens, block), lambda i, place: (0, place[0] * steps + i)),
        ),
        out_shape=jax.ShapeDtypeStruct((tokens, columns), jnp.bfloat16),
        input_output_aliases=aliases,
        compiler_params=params(("arbitrary",)),
        cost_estimate=cost(2 * tokens * channels * width, 2 * channels * (tokens + width)),
        name="project",
    )(place, *operands)


def per_device(lin_pre, gate_pre, w_depth, ln_gain, ln_shift, w_out):
    dp, sp = lax.axis_size("dp"), lax.axis_size("sp")
    chips = dp // 2
    mine = lax.axis_index("dp")
    spot = lax.axis_index("sp") % 4
    swap = [(i, i ^ 1) for i in range(dp)]
    quarter = w_out.shape[0] // 4

    def unit_of(which):
        return lax.dynamic_slice_in_dim(w_out, which * quarter, quarter, axis=0)

    def to_sibling(x):
        return lax.ppermute(x, "dp", swap)

    direct_a, direct_b = [], []
    head_unit, last_unit = unit_of(spot), unit_of(3 - spot)
    hops = [
        [(i, (i // 2 + k) % chips * 2 + i % 2) for i in range(dp)] for k in range(1, chips)
    ]
    for perm in hops:
        direct_a.append(lax.ppermute(head_unit, "dp", perm))
    for perm in hops:
        direct_b.append(lax.ppermute(last_unit, "dp", perm))
    sibling = to_sibling(w_out)

    glu, head, tail = gated(lin_pre, gate_pre)
    ends = sp - 1
    before = lax.ppermute(tail, "sp", [(i, i + 1) for i in range(ends)])
    after = lax.ppermute(head, "sp", [(i + 1, i) for i in range(ends)])
    gain, shift = ln_gain[None, :], ln_shift[None, :]
    act = activated_inner(glu, w_depth, gain, shift)
    before, after, act = lax.optimization_barrier((before, after, act))
    act = activated_outer(before, after, glu, w_depth, gain, shift, act)

    direct_a, act = lax.optimization_barrier((direct_a, act))
    columns = w_out.shape[1] * dp
    units = (spot, 3 - spot, spot ^ 1, spot ^ 2)
    by_x = [lax.ppermute(a, "sp", [(i, i ^ 1) for i in range(sp)]) for a in direct_a]
    by_z = [lax.ppermute(a, "sp", [(i, i ^ 2) for i in range(sp)]) for a in direct_a]
    swapped_a = [to_sibling(a) for a in direct_a]
    out = project(act, [w_out], (), mine, columns, None)
    out = project(act, [sibling], (), mine ^ 1, columns, out)
    by_x, by_z, direct_b, swapped_a, out = lax.optimization_barrier(
        (by_x, by_z, direct_b, swapped_a, out)
    )
    for k in range(1, chips):
        source = (mine // 2 - k) % chips * 2 + mine % 2
        near = [direct_a[k - 1], direct_b[k - 1], by_x[k - 1], by_z[k - 1]]
        far = [swapped_a[k - 1]] + [to_sibling(x) for x in near[1:]]
        out = project(act, near, units, source, columns, out)
        out = project(act, far, units, source ^ 1, columns, out)
    return out


def solution(mesh):
    in_specs = (P(None, ("dp", "sp")), P(None, ("dp", "sp")), P(), P(), P(), P(None, "dp"))
    out_specs = P(("dp", "sp"), None)
    return jax.shard_map(
        per_device, mesh=mesh, in_specs=in_specs, out_specs=out_specs, check_vma=False
    )
```

```python
import functools

import jax
import jax.numpy as jnp
from jax import lax
from jax.experimental import pallas as pl
from jax.experimental.pallas import tpu as pltpu
from jax.sharding import PartitionSpec as P


LANES = 128
EDGE = 16
EPS = 1e-05


def params(semantics=None):
    return pltpu.CompilerParams(dimension_semantics=semantics, vmem_limit_bytes=16 << 20)


def cost(flops, nbytes):
    return pl.CostEstimate(flops=flops, transcendentals=0, bytes_accessed=nbytes)


def glu_body(lin_ref, gate_ref, out_ref, head_ref, tail_ref):
    gate = gate_ref[...].astype(jnp.float32)
    glu = (lin_ref[...].astype(jnp.float32) * jax.nn.sigmoid(gate)).T.astype(jnp.bfloat16)
    out_ref[...] = glu
    head_ref[...] = glu[:EDGE]
    tail_ref[...] = glu[glu.shape[0] - EDGE :]


def gated(lin_pre, gate_pre):
    channels, tokens = lin_pre.shape
    block = 256
    edge = pl.BlockSpec((EDGE, block), lambda i: (0, i))
    return pl.pallas_call(
        glu_body,
        grid=(channels // block,),
        in_specs=[pl.BlockSpec((block, tokens), lambda i: (i, 0))] * 2,
        out_specs=[pl.BlockSpec((tokens, block), lambda i: (0, i)), edge, edge],
        out_shape=[
            jax.ShapeDtypeStruct((tokens, channels), jnp.bfloat16),
            jax.ShapeDtypeStruct((EDGE, channels), jnp.bfloat16),
            jax.ShapeDtypeStruct((EDGE, channels), jnp.bfloat16),
        ],
        compiler_params=params(("arbitrary",)),
        cost_estimate=cost(20 * channels * tokens, 6 * channels * tokens),
        name="glu",
    )(lin_pre, gate_pre)


def conv_norm(cells, w_ref, gain_ref, shift_ref, mixed, start, tiles, store):
    blocks = cells.shape[0]
    span = 8 * tiles
    channels = blocks * LANES
    taps = w_ref.shape[0]

    def one_block(block, total):
        lanes = pl.ds(pl.multiple_of(block * LANES, LANES), LANES)
        running = [jnp.zeros((span, LANES), jnp.float32) for _ in range(2)]
        turn = 0
        lead = EDGE - (taps - 1) // 2
        for phase in range(8):
            window = cells[block, pl.ds(start - EDGE + phase, span + 8 * 3), :]
            for whole in range(4):
                tap = 8 * whole + phase - lead
                if 0 <= tap < taps:
                    weight = w_ref[pl.ds(tap, 1), lanes]
                    running[turn] = running[turn] + weight * window[8 * whole : 8 * whole + span]
                    turn = 1 - turn
        value = (running[0] + running[1]).astype(jnp.bfloat16).astype(jnp.float32)
        mixed[block, pl.ds(0, span), :] = value
        return total + value

    zeros = jnp.zeros((span, LANES), jnp.float32)
    total = lax.fori_loop(0, blocks, one_block, zeros)
    mean = jnp.broadcast_to(jnp.sum(total, axis=1, keepdims=True) / channels, (span, LANES))

    square = zeros
    for block in range(blocks):
        square = square + jnp.square(mixed[block, pl.ds(0, span), :] - mean)
    variance = jnp.sum(square, axis=1, keepdims=True) / channels
    scale = jnp.broadcast_to(lax.rsqrt(variance + EPS), (span, LANES))
    for block in range(blocks):
        lanes = pl.ds(block * LANES, LANES)
        normed = (mixed[block, pl.ds(0, span), :] - mean) * scale
        normed = normed * gain_ref[:, lanes] + shift_ref[:, lanes]
        store(lanes, (normed * jax.nn.sigmoid(normed)).astype(jnp.bfloat16))


def inner_body(tiles, glu_ref, w_ref, gain_ref, shift_ref, out_ref, cells, mixed):
    blocks = cells.shape[0]
    for block in range(blocks):
        cells[block] = glu_ref[:, pl.ds(block * LANES, LANES)].astype(jnp.float32)
    span = 8 * tiles

    def chunk(i, carry):
        start = pl.multiple_of(EDGE + i * span, 8)

        def store(lanes, value):
            out_ref[pl.ds(start, span), lanes] = value

        conv_norm(cells, w_ref, gain_ref, shift_ref, mixed, start, tiles, store)
        return carry

    lax.fori_loop(0, (glu_ref.shape[0] - 2 * EDGE) // span, chunk, 0)


def outer_body(before_ref, after_ref, glu_ref, w_ref, gain_ref, shift_ref, _, out_ref, cells, mixed):
    side = pl.program_id(0)
    blocks = cells.shape[0]
    for block in range(blocks):
        lanes = pl.ds(block * LANES, LANES)
        own = glu_ref[:, lanes].astype(jnp.float32)
        halo = jnp.where(side == 0, before_ref[:, lanes], after_ref[:, lanes]).astype(jnp.float32)
        cells[block, pl.ds(EDGE, 2 * EDGE), :] = jnp.where(side == 0, own, 0.0)
        cells[block, pl.ds(0, EDGE), :] = jnp.where(side == 0, halo, own[:EDGE])
        cells[block, pl.ds(EDGE, EDGE), :] = jnp.where(side == 0, own[:EDGE], own[EDGE:])
        cells[block, pl.ds(2 * EDGE, EDGE), :] = jnp.where(side == 0, own[EDGE:], halo)

    def store(lanes, value):
        out_ref[:, lanes] = value

    conv_norm(cells, w_ref, gain_ref, shift_ref, mixed, EDGE, EDGE // 8, store)


def activated_inner(glu, w_depth, gain, shift):
    tokens, channels = glu.shape
    inner = (tokens - 2 * EDGE) // 16
    tiles = 2 * max(n for n in range(1, 5) if inner % n == 0)
    blocks = channels // LANES
    return pl.pallas_call(
        functools.partial(inner_body, tiles),
        out_shape=jax.ShapeDtypeStruct((tokens, channels), jnp.bfloat16),
        scratch_shapes=[
            pltpu.VMEM((blocks, tokens, LANES), jnp.float32),
            pltpu.VMEM((blocks, 8 * tiles, LANES), jnp.float32),
        ],
        compiler_params=params(),
        cost_estimate=cost(80 * channels * tokens, 4 * channels * tokens),
        name="conv_inner",
    )(glu, w_depth, gain, shift)


def activated_outer(before, after, glu, w_depth, gain, shift, act):
    tokens, channels = glu.shape
    blocks = channels // LANES
    whole = pl.BlockSpec((EDGE, channels), lambda i: (0, 0))
    row = pl.BlockSpec((1, channels), lambda i: (0, 0))
    last = tokens // EDGE - 1
    return pl.pallas_call(
        outer_body,
        grid=(2,),
        in_specs=[
            whole,
            whole,
            pl.BlockSpec((2 * EDGE, channels), lambda i: (i * (tokens // (2 * EDGE) - 1), 0)),
            pl.BlockSpec(w_depth.shape, lambda i: (0, 0)),
            row,
            row,
            pl.BlockSpec(memory_space=pl.ANY),
        ],
        out_specs=pl.BlockSpec((EDGE, channels), lambda i: (i * last, 0)),
        out_shape=jax.ShapeDtypeStruct((tokens, channels), jnp.bfloat16),
        scratch_shapes=[
            pltpu.VMEM((blocks, 3 * EDGE, LANES), jnp.float32),
            pltpu.VMEM((blocks, EDGE, LANES), jnp.float32),
        ],
        input_output_aliases={6: 0},
        compiler_params=params(("arbitrary",)),
        cost_estimate=cost(80 * channels * 2 * EDGE, 8 * channels * EDGE),
        name="conv_outer",
    )(before, after, glu, w_depth, gain, shift, act)


WHOLE = pl.BlockSpec(memory_space=pltpu.VMEM)
STAY = pl.BlockSpec(memory_space=pltpu.HBM)
TABLE = pl.BlockSpec(memory_space=pltpu.SMEM)


def quarters_body(place_ref, w_ref, *refs):
    outs, sems = refs[:-1], refs[-1]
    rows = outs[0].shape[0]
    copies = [
        pltpu.make_async_copy(w_ref.at[pl.ds(place_ref[i] * rows, rows), :], out, sems.at[i])
        for i, out in enumerate(outs)
    ]
    for copy in copies:
        copy.start()
    for copy in copies:
        copy.wait()


def quarters(w_out, units):
    shape = jax.ShapeDtypeStruct((w_out.shape[0] // 4, w_out.shape[1]), w_out.dtype)
    return pl.pallas_call(
        quarters_body,
        in_specs=[TABLE, STAY],
        out_specs=[WHOLE] * len(units),
        out_shape=[shape] * len(units),
        scratch_shapes=[pltpu.SemaphoreType.DMA((len(units),))],
        compiler_params=params(),
        name="quarters",
    )(jnp.stack(units), pltpu.with_memory_space_constraint(w_out, pltpu.HBM))


def project_body(place_ref, act_ref, *refs):
    chunks, out_ref = refs[:-1], refs[-1]
    rows = chunks[0].shape[0]
    total = None
    for i, chunk in enumerate(chunks):
        if len(chunks) == 1:
            part = act_ref[...]
        else:
            part = act_ref[:, pl.ds(pl.multiple_of(place_ref[i] * rows, LANES), rows)]
        term = jnp.dot(part, chunk[...], preferred_element_type=jnp.float32)
        total = term if total is None else total + term
    out_ref[...] = total.astype(jnp.bfloat16)


def project(act, chunks, units):
    tokens, channels = act.shape
    width = chunks[0].shape[1]
    return pl.pallas_call(
        project_body,
        in_specs=[TABLE] + [WHOLE] * (1 + len(chunks)),
        out_specs=WHOLE,
        out_shape=jax.ShapeDtypeStruct((tokens, width), jnp.bfloat16),
        compiler_params=params(),
        cost_estimate=cost(2 * tokens * channels * width, 2 * channels * (tokens + width)),
        name="project",
    )(jnp.stack(units), act, *chunks)


def collect_body(place_ref, *refs):
    pieces, out_ref, sems = refs[:-2], refs[-2], refs[-1]
    width = pieces[0].shape[1]
    copies = []
    for i, piece in enumerate(pieces):
        at = pl.multiple_of(place_ref[i] * width, LANES)
        copies.append(pltpu.make_async_copy(piece, out_ref.at[:, pl.ds(at, width)], sems.at[i]))
    for copy in copies:
        copy.start()
    for copy in copies:
        copy.wait()


def collect(pieces, shards):
    tokens, width = pieces[0].shape
    return pl.pallas_call(
        collect_body,
        in_specs=[TABLE] + [WHOLE] * len(pieces),
        out_specs=STAY,
        out_shape=jax.ShapeDtypeStruct((tokens, width * len(pieces)), jnp.bfloat16),
        scratch_shapes=[pltpu.SemaphoreType.DMA((len(pieces),))],
        compiler_params=params(),
        name="collect",
    )(jnp.stack(shards), *pieces)


def per_device(lin_pre, gate_pre, w_depth, ln_gain, ln_shift, w_out):
    dp, sp = lax.axis_size("dp"), lax.axis_size("sp")
    chips = dp // 2
    mine = lax.axis_index("dp")
    spot = lax.axis_index("sp") % 4

    def to_sibling(x):
        return lax.ppermute(x, "dp", [(i, i ^ 1) for i in range(dp)])

    def to_near(x, bit):
        return lax.ppermute(x, "sp", [(i, i ^ bit) for i in range(sp)])

    first, second = quarters(w_out, (spot, 3 - spot))
    hops = [
        [(i, (i // 2 + k) % chips * 2 + i % 2) for i in range(dp)] for k in range(1, chips)
    ]
    direct_a = [lax.ppermute(first, "dp", perm) for perm in hops]
    direct_b = [lax.ppermute(second, "dp", perm) for perm in hops]

    glu, head, tail = gated(lin_pre, gate_pre)
    ends = sp - 1
    before = lax.ppermute(tail, "sp", [(i, i + 1) for i in range(ends)])
    after = lax.ppermute(head, "sp", [(i + 1, i) for i in range(ends)])
    gain, shift = ln_gain[None, :], ln_shift[None, :]
    act = activated_inner(glu, w_depth, gain, shift)
    direct_a, act = lax.optimization_barrier((direct_a, act))
    by_x = [to_near(a, 1) for a in direct_a]
    by_z = [to_near(a, 2) for a in direct_a]
    before, after, act = lax.optimization_barrier((before, after, act))
    act = activated_outer(before, after, glu, w_depth, gain, shift, act)

    act_far = to_sibling(act)
    pieces, shards = [project(act, [w_out], (spot,))], [mine]
    own_far = project(act_far, [w_out], (spot,))
    received = [to_sibling(own_far)]
    by_x, by_z, direct_b, act_far, act, pieces = lax.optimization_barrier(
        (by_x, by_z, direct_b, act_far, act, pieces)
    )
    units = (spot, 3 - spot, spot ^ 1, spot ^ 2)
    for k in range(1, chips):
        near = [direct_a[k - 1], direct_b[k - 1], by_x[k - 1], by_z[k - 1]]
        other_far = project(act_far, near, units)
        received.append(to_sibling(other_far))
        pieces.append(project(act, near, units))
        shards.append((mine // 2 - k) % chips * 2 + mine % 2)
    return collect(pieces + received, shards + [shard ^ 1 for shard in shards])


def solution(mesh):
    in_specs = (P(None, ("dp", "sp")), P(None, ("dp", "sp")), P(), P(), P(), P(None, "dp"))
    out_specs = P(("dp", "sp"), None)
    return jax.shard_map(
        per_device, mesh=mesh, in_specs=in_specs, out_specs=out_specs, check_vma=False
    )
```

```python
import functools

import jax
import jax.numpy as jnp
from jax import lax
from jax.experimental import pallas as pl
from jax.experimental.pallas import tpu as pltpu
from jax.sharding import PartitionSpec as P


LANES = 128
EDGE = 16
EPS = 1e-05


def params(semantics=None):
    return pltpu.CompilerParams(dimension_semantics=semantics, vmem_limit_bytes=8 << 20)


def far_memory(x):
    return pltpu.with_memory_space_constraint(x, pltpu.HBM)


def cost(flops, nbytes):
    return pl.CostEstimate(flops=flops, transcendentals=0, bytes_accessed=nbytes)


def glu_body(lin_ref, gate_ref, out_ref, head_ref, tail_ref):
    gate = gate_ref[...].astype(jnp.float32)
    glu = (lin_ref[...].astype(jnp.float32) * jax.nn.sigmoid(gate)).T.astype(jnp.bfloat16)
    out_ref[...] = glu
    head_ref[...] = glu[:EDGE]
    tail_ref[...] = glu[glu.shape[0] - EDGE :]


def gated(lin_pre, gate_pre):
    channels, tokens = lin_pre.shape
    block = 256
    edge = pl.BlockSpec((EDGE, block), lambda i: (0, i))
    return pl.pallas_call(
        glu_body,
        grid=(channels // block,),
        in_specs=[pl.BlockSpec((block, tokens), lambda i: (i, 0))] * 2,
        out_specs=[pl.BlockSpec((tokens, block), lambda i: (0, i)), edge, edge],
        out_shape=[
            jax.ShapeDtypeStruct((tokens, channels), jnp.bfloat16),
            jax.ShapeDtypeStruct((EDGE, channels), jnp.bfloat16),
            jax.ShapeDtypeStruct((EDGE, channels), jnp.bfloat16),
        ],
        compiler_params=params(("arbitrary",)),
        cost_estimate=cost(20 * channels * tokens, 6 * channels * tokens),
        name="glu",
    )(lin_pre, gate_pre)


def conv_norm(cells, w_ref, gain_ref, shift_ref, mixed, start, tiles, store):
    blocks = cells.shape[0]
    span = 8 * tiles
    channels = blocks * LANES
    taps = w_ref.shape[0]

    def one_block(block, total):
        lanes = pl.ds(pl.multiple_of(block * LANES, LANES), LANES)
        running = [jnp.zeros((span, LANES), jnp.float32) for _ in range(2)]
        turn = 0
        lead = EDGE - (taps - 1) // 2
        for phase in range(8):
            window = cells[block, pl.ds(start - EDGE + phase, span + 8 * 3), :]
            for whole in range(4):
                tap = 8 * whole + phase - lead
                if 0 <= tap < taps:
                    weight = w_ref[pl.ds(tap, 1), lanes]
                    running[turn] = running[turn] + weight * window[8 * whole : 8 * whole + span]
                    turn = 1 - turn
        value = (running[0] + running[1]).astype(jnp.bfloat16).astype(jnp.float32)
        mixed[block, pl.ds(0, span), :] = value
        return total + value

    zeros = jnp.zeros((span, LANES), jnp.float32)
    total = lax.fori_loop(0, blocks, one_block, zeros)
    mean = jnp.broadcast_to(jnp.sum(total, axis=1, keepdims=True) / channels, (span, LANES))

    square = zeros
    for block in range(blocks):
        square = square + jnp.square(mixed[block, pl.ds(0, span), :] - mean)
    variance = jnp.sum(square, axis=1, keepdims=True) / channels
    scale = jnp.broadcast_to(lax.rsqrt(variance + EPS), (span, LANES))
    for block in range(blocks):
        lanes = pl.ds(block * LANES, LANES)
        normed = (mixed[block, pl.ds(0, span), :] - mean) * scale
        normed = normed * gain_ref[:, lanes] + shift_ref[:, lanes]
        store(lanes, (normed * jax.nn.sigmoid(normed)).astype(jnp.bfloat16))


def inner_body(tiles, glu_ref, w_ref, gain_ref, shift_ref, out_ref, cells, mixed):
    blocks = cells.shape[0]
    for block in range(blocks):
        cells[block] = glu_ref[:, pl.ds(block * LANES, LANES)].astype(jnp.float32)
    span = 8 * tiles

    def chunk(i, carry):
        start = pl.multiple_of(EDGE + i * span, 8)

        def store(lanes, value):
            out_ref[pl.ds(start, span), lanes] = value

        conv_norm(cells, w_ref, gain_ref, shift_ref, mixed, start, tiles, store)
        return carry

    lax.fori_loop(0, (glu_ref.shape[0] - 2 * EDGE) // span, chunk, 0)


def outer_body(before_ref, after_ref, glu_ref, w_ref, gain_ref, shift_ref, _, out_ref, cells, mixed):
    side = pl.program_id(0)
    blocks = cells.shape[0]
    for block in range(blocks):
        lanes = pl.ds(block * LANES, LANES)
        own = glu_ref[:, lanes].astype(jnp.float32)
        halo = jnp.where(side == 0, before_ref[:, lanes], after_ref[:, lanes]).astype(jnp.float32)
        cells[block, pl.ds(EDGE, 2 * EDGE), :] = jnp.where(side == 0, own, 0.0)
        cells[block, pl.ds(0, EDGE), :] = jnp.where(side == 0, halo, own[:EDGE])
        cells[block, pl.ds(EDGE, EDGE), :] = jnp.where(side == 0, own[:EDGE], own[EDGE:])
        cells[block, pl.ds(2 * EDGE, EDGE), :] = jnp.where(side == 0, own[EDGE:], halo)

    def store(lanes, value):
        out_ref[:, lanes] = value

    conv_norm(cells, w_ref, gain_ref, shift_ref, mixed, EDGE, EDGE // 8, store)


def activated_inner(glu, w_depth, gain, shift):
    tokens, channels = glu.shape
    inner = (tokens - 2 * EDGE) // 16
    tiles = 2 * max(n for n in range(1, 5) if inner % n == 0)
    blocks = channels // LANES
    return pl.pallas_call(
        functools.partial(inner_body, tiles),
        out_shape=jax.ShapeDtypeStruct((tokens, channels), jnp.bfloat16),
        scratch_shapes=[
            pltpu.VMEM((blocks, tokens, LANES), jnp.float32),
            pltpu.VMEM((blocks, 8 * tiles, LANES), jnp.float32),
        ],
        compiler_params=params(),
        cost_estimate=cost(80 * channels * tokens, 4 * channels * tokens),
        name="conv_inner",
    )(glu, w_depth, gain, shift)


def activated_outer(before, after, glu, w_depth, gain, shift, act):
    tokens, channels = glu.shape
    blocks = channels // LANES
    whole = pl.BlockSpec((EDGE, channels), lambda i: (0, 0))
    row = pl.BlockSpec((1, channels), lambda i: (0, 0))
    last = tokens // EDGE - 1
    return pl.pallas_call(
        outer_body,
        grid=(2,),
        in_specs=[
            whole,
            whole,
            pl.BlockSpec((2 * EDGE, channels), lambda i: (i * (tokens // (2 * EDGE) - 1), 0)),
            pl.BlockSpec(w_depth.shape, lambda i: (0, 0)),
            row,
            row,
            pl.BlockSpec(memory_space=pl.ANY),
        ],
        out_specs=pl.BlockSpec((EDGE, channels), lambda i: (i * last, 0)),
        out_shape=jax.ShapeDtypeStruct((tokens, channels), jnp.bfloat16),
        scratch_shapes=[
            pltpu.VMEM((blocks, 3 * EDGE, LANES), jnp.float32),
            pltpu.VMEM((blocks, EDGE, LANES), jnp.float32),
        ],
        input_output_aliases={6: 0},
        compiler_params=params(("arbitrary",)),
        cost_estimate=cost(80 * channels * 2 * EDGE, 8 * channels * EDGE),
        name="conv_outer",
    )(before, after, glu, w_depth, gain, shift, act)


WHOLE = pl.BlockSpec(memory_space=pltpu.VMEM)
STAY = pl.BlockSpec(memory_space=pltpu.HBM)
TABLE = pl.BlockSpec(memory_space=pltpu.SMEM)


def cut_body(place_ref, w_ref, *refs):
    outs, sems = refs[:-1], refs[-1]
    copies = []
    for i, out in enumerate(outs):
        start = pl.multiple_of(place_ref[i] * LANES, LANES)
        rows = w_ref.at[pl.ds(start, out.shape[0]), :]
        copies.append(pltpu.make_async_copy(rows, out, sems.at[i]))
    for copy in copies:
        copy.start()
    for copy in copies:
        copy.wait()


def cut(w_out, rows, places):
    return pl.pallas_call(
        cut_body,
        in_specs=[TABLE, STAY],
        out_specs=[WHOLE] * len(places),
        out_shape=[jax.ShapeDtypeStruct((rows, w_out.shape[1]), w_out.dtype)] * len(places),
        scratch_shapes=[pltpu.SemaphoreType.DMA((len(places),))],
        compiler_params=params(),
        name="cut",
    )(jnp.stack(places), far_memory(w_out))


def project_body(place_ref, act_ref, *refs):
    chunks, out_ref = refs[:-1], refs[-1]
    total = None
    for i, chunk in enumerate(chunks):
        if len(chunks) == 1:
            part = act_ref[...]
        else:
            start = pl.multiple_of(place_ref[i] * LANES, LANES)
            part = act_ref[:, pl.ds(start, chunk.shape[0])]
        term = jnp.dot(part, chunk[...], preferred_element_type=jnp.float32)
        total = term if total is None else total + term
    out_ref[...] = total.astype(jnp.bfloat16)


def project(act, chunks, places):
    tokens, channels = act.shape
    width = chunks[0].shape[1]
    return pl.pallas_call(
        project_body,
        in_specs=[TABLE] + [WHOLE] * (1 + len(chunks)),
        out_specs=WHOLE,
        out_shape=jax.ShapeDtypeStruct((tokens, width), jnp.bfloat16),
        compiler_params=params(),
        cost_estimate=cost(2 * tokens * channels * width, 2 * channels * (tokens + width)),
        name="project",
    )(jnp.stack(places), act, *chunks)


def collect_body(place_ref, *refs):
    pieces, out_ref, sems = refs[:-2], refs[-2], refs[-1]
    width = pieces[0].shape[1]
    copies = []
    for i, piece in enumerate(pieces):
        at = pl.multiple_of(place_ref[i] * width, LANES)
        copies.append(pltpu.make_async_copy(piece, out_ref.at[:, pl.ds(at, width)], sems.at[i]))
    for copy in copies:
        copy.start()
    for copy in copies:
        copy.wait()


def collect(pieces, shards):
    tokens, width = pieces[0].shape
    return pl.pallas_call(
        collect_body,
        in_specs=[TABLE] + [WHOLE] * len(pieces),
        out_specs=STAY,
        out_shape=jax.ShapeDtypeStruct((tokens, width * len(pieces)), jnp.bfloat16),
        scratch_shapes=[pltpu.SemaphoreType.DMA((len(pieces),))],
        compiler_params=params(),
        name="collect",
    )(jnp.stack(shards), *pieces)


def per_device(lin_pre, gate_pre, w_depth, ln_gain, ln_shift, w_out):
    dp, sp = lax.axis_size("dp"), lax.axis_size("sp")
    chips = dp // 2
    mine = lax.axis_index("dp")
    spot = lax.axis_index("sp") % 4

    def to_sibling(x):
        return lax.ppermute(x, "dp", [(i, i ^ 1) for i in range(dp)])

    def to_near(x, bit):
        return lax.ppermute(x, "sp", [(i, i ^ bit) for i in range(sp)])

    quarter = w_out.shape[0] // 4
    half = quarter // 2
    tiles = quarter // LANES

    def halves(unit):
        return [unit * tiles, unit * tiles + tiles // 2]

    hops = [
        [(i, (i // 2 + k) % chips * 2 + i % 2) for i in range(dp)] for k in range(1, chips)
    ]
    firsts = cut(w_out, half, halves(spot))
    direct_a1 = [lax.ppermute(firsts[0], "dp", perm) for perm in hops]
    direct_a2 = [lax.ppermute(firsts[1], "dp", perm) for perm in hops]
    (second,) = cut(w_out, quarter, ((3 - spot) * tiles,))
    direct_b = [lax.ppermute(second, "dp", perm) for perm in hops]

    glu, head, tail = gated(lin_pre, gate_pre)
    ends = sp - 1
    before = lax.ppermute(tail, "sp", [(i, i + 1) for i in range(ends)])
    after = lax.ppermute(head, "sp", [(i + 1, i) for i in range(ends)])
    gain, shift = ln_gain[None, :], ln_shift[None, :]
    act = activated_inner(glu, w_depth, gain, shift)
    by_x1 = [to_near(part, 1) for part in direct_a1]
    by_z1 = [to_near(part, 2) for part in direct_a1]
    direct_a2, act = lax.optimization_barrier((direct_a2, act))
    by_x2 = [to_near(part, 1) for part in direct_a2]
    by_z2 = [to_near(part, 2) for part in direct_a2]
    before, after, act = lax.optimization_barrier((before, after, act))
    act = activated_outer(before, after, glu, w_depth, gain, shift, act)

    act_far = to_sibling(act)
    pieces, shards = [project(act, [far_memory(w_out)], (spot,))], [mine]
    own_far = project(act_far, [far_memory(w_out)], (spot,))
    received = [to_sibling(own_far)]
    places = halves(spot) + [(3 - spot) * tiles] + halves(spot ^ 1) + halves(spot ^ 2)
    arrivals = [direct_a1, direct_a2, direct_b, by_x1, by_x2, by_z1, by_z2]
    for k in range(1, chips):
        near = [arrival[k - 1] for arrival in arrivals]
        other_far = project(act_far, near, places)
        received.append(to_sibling(other_far))
        pieces.append(project(act, near, places))
        shards.append((mine // 2 - k) % chips * 2 + mine % 2)
    return collect(pieces + received, shards + [shard ^ 1 for shard in shards])


def solution(mesh):
    in_specs = (P(None, ("dp", "sp")), P(None, ("dp", "sp")), P(), P(), P(), P(None, "dp"))
    out_specs = P(("dp", "sp"), None)
    return jax.shard_map(
        per_device, mesh=mesh, in_specs=in_specs, out_specs=out_specs, check_vma=False
    )
```

```python
import functools

import jax
import jax.numpy as jnp
from jax import lax
from jax.experimental import pallas as pl
from jax.experimental.pallas import tpu as pltpu
from jax.sharding import PartitionSpec as P


LANES = 128
EDGE = 16
EPS = 1e-05
WHOLE = pl.BlockSpec(memory_space=pltpu.VMEM)
STAY = pl.BlockSpec(memory_space=pltpu.HBM)
TABLE = pl.BlockSpec(memory_space=pltpu.SMEM)


def params(semantics=None):
    return pltpu.CompilerParams(dimension_semantics=semantics, vmem_limit_bytes=8 << 20)


def far_memory(x):
    return pltpu.with_memory_space_constraint(x, pltpu.HBM)


def cost(flops, nbytes):
    return pl.CostEstimate(flops=flops, transcendentals=0, bytes_accessed=nbytes)


def glu_body(parity_ref, lin_ref, gate_ref, out_ref, near_ref, next_ref):
    gate = gate_ref[...].astype(jnp.float32)
    glu = (lin_ref[...].astype(jnp.float32) * jax.nn.sigmoid(gate)).T.astype(jnp.bfloat16)
    out_ref[...] = glu
    head, tail = glu[:EDGE], glu[glu.shape[0] - EDGE :]
    even = parity_ref[0] == 0
    near_ref[...] = jnp.where(even, tail, head)
    next_ref[...] = jnp.where(even, head, tail)


def gated(parity, lin_pre, gate_pre):
    channels, tokens = lin_pre.shape
    block = 256
    edge = pl.BlockSpec((EDGE, block), lambda i: (0, i))
    return pl.pallas_call(
        glu_body,
        grid=(channels // block,),
        in_specs=[TABLE] + [pl.BlockSpec((block, tokens), lambda i: (i, 0))] * 2,
        out_specs=[pl.BlockSpec((tokens, block), lambda i: (0, i)), edge, edge],
        out_shape=[
            jax.ShapeDtypeStruct((tokens, channels), jnp.bfloat16),
            jax.ShapeDtypeStruct((EDGE, channels), jnp.bfloat16),
            jax.ShapeDtypeStruct((EDGE, channels), jnp.bfloat16),
        ],
        compiler_params=params(("arbitrary",)),
        cost_estimate=cost(20 * channels * tokens, 6 * channels * tokens),
        name="glu",
    )(parity, lin_pre, gate_pre)


def conv_norm(cells, w_ref, gain_ref, shift_ref, mixed, start, tiles, store):
    blocks = cells.shape[0]
    span = 8 * tiles
    channels = blocks * LANES
    taps = w_ref.shape[0]

    def one_block(block, total):
        lanes = pl.ds(pl.multiple_of(block * LANES, LANES), LANES)
        running = [jnp.zeros((span, LANES), jnp.float32) for _ in range(2)]
        turn = 0
        lead = EDGE - (taps - 1) // 2
        for phase in range(8):
            window = cells[block, pl.ds(start - EDGE + phase, span + 8 * 3), :]
            for whole in range(4):
                tap = 8 * whole + phase - lead
                if 0 <= tap < taps:
                    weight = w_ref[pl.ds(tap, 1), lanes]
                    running[turn] = running[turn] + weight * window[8 * whole : 8 * whole + span]
                    turn = 1 - turn
        value = (running[0] + running[1]).astype(jnp.bfloat16).astype(jnp.float32)
        mixed[block, pl.ds(0, span), :] = value
        return total + value

    zeros = jnp.zeros((span, LANES), jnp.float32)
    total = lax.fori_loop(0, blocks, one_block, zeros)
    mean = jnp.broadcast_to(jnp.sum(total, axis=1, keepdims=True) / channels, (span, LANES))

    square = zeros
    for block in range(blocks):
        square = square + jnp.square(mixed[block, pl.ds(0, span), :] - mean)
    variance = jnp.sum(square, axis=1, keepdims=True) / channels
    scale = jnp.broadcast_to(lax.rsqrt(variance + EPS), (span, LANES))
    for block in range(blocks):
        lanes = pl.ds(block * LANES, LANES)
        normed = (mixed[block, pl.ds(0, span), :] - mean) * scale
        normed = normed * gain_ref[:, lanes] + shift_ref[:, lanes]
        store(lanes, (normed * jax.nn.sigmoid(normed)).astype(jnp.bfloat16))


def inner_body(tiles, glu_ref, w_ref, gain_ref, shift_ref, out_ref, cells, mixed):
    blocks = cells.shape[0]
    for block in range(blocks):
        cells[block] = glu_ref[:, pl.ds(block * LANES, LANES)].astype(jnp.float32)
    span = 8 * tiles

    def chunk(i, carry):
        start = pl.multiple_of(EDGE + i * span, 8)

        def store(lanes, value):
            out_ref[pl.ds(start, span), lanes] = value

        conv_norm(cells, w_ref, gain_ref, shift_ref, mixed, start, tiles, store)
        return carry

    lax.fori_loop(0, (glu_ref.shape[0] - 2 * EDGE) // span, chunk, 0)


def outer_body(parity_ref, near_ref, next_ref, glu_ref, w_ref, gain_ref, shift_ref, _, out_ref, cells, mixed):
    side = pl.program_id(0)
    blocks = cells.shape[0]
    for block in range(blocks):
        lanes = pl.ds(block * LANES, LANES)
        own = glu_ref[:, lanes].astype(jnp.float32)
        halo = jnp.where(side != parity_ref[0], near_ref[:, lanes], next_ref[:, lanes])
        halo = halo.astype(jnp.float32)
        cells[block, pl.ds(EDGE, 2 * EDGE), :] = jnp.where(side == 0, own, 0.0)
        cells[block, pl.ds(0, EDGE), :] = jnp.where(side == 0, halo, own[:EDGE])
        cells[block, pl.ds(EDGE, EDGE), :] = jnp.where(side == 0, own[:EDGE], own[EDGE:])
        cells[block, pl.ds(2 * EDGE, EDGE), :] = jnp.where(side == 0, own[EDGE:], halo)

    def store(lanes, value):
        out_ref[:, lanes] = value

    conv_norm(cells, w_ref, gain_ref, shift_ref, mixed, EDGE, EDGE // 8, store)


def activated_inner(glu, w_depth, gain, shift):
    tokens, channels = glu.shape
    inner = (tokens - 2 * EDGE) // 16
    tiles = 2 * max(n for n in range(1, 5) if inner % n == 0)
    blocks = channels // LANES
    return pl.pallas_call(
        functools.partial(inner_body, tiles),
        out_shape=jax.ShapeDtypeStruct((tokens, channels), jnp.bfloat16),
        scratch_shapes=[
            pltpu.VMEM((blocks, tokens, LANES), jnp.float32),
            pltpu.VMEM((blocks, 8 * tiles, LANES), jnp.float32),
        ],
        compiler_params=params(),
        cost_estimate=cost(80 * channels * tokens, 4 * channels * tokens),
        name="conv_inner",
    )(glu, w_depth, gain, shift)


def activated_outer(parity, near, ahead, glu, w_depth, gain, shift, act):
    tokens, channels = glu.shape
    blocks = channels // LANES
    whole = pl.BlockSpec((EDGE, channels), lambda i: (0, 0))
    row = pl.BlockSpec((1, channels), lambda i: (0, 0))
    last = tokens // EDGE - 1
    return pl.pallas_call(
        outer_body,
        grid=(2,),
        in_specs=[
            TABLE,
            whole,
            whole,
            pl.BlockSpec((2 * EDGE, channels), lambda i: (i * (tokens // (2 * EDGE) - 1), 0)),
            pl.BlockSpec(w_depth.shape, lambda i: (0, 0)),
            row,
            row,
            pl.BlockSpec(memory_space=pl.ANY),
        ],
        out_specs=pl.BlockSpec((EDGE, channels), lambda i: (i * last, 0)),
        out_shape=jax.ShapeDtypeStruct((tokens, channels), jnp.bfloat16),
        scratch_shapes=[
            pltpu.VMEM((blocks, 3 * EDGE, LANES), jnp.float32),
            pltpu.VMEM((blocks, EDGE, LANES), jnp.float32),
        ],
        input_output_aliases={7: 0},
        compiler_params=params(("arbitrary",)),
        cost_estimate=cost(80 * channels * 2 * EDGE, 8 * channels * EDGE),
        name="conv_outer",
    )(parity, near, ahead, glu, w_depth, gain, shift, act)


def cut_body(place_ref, w_ref, *refs):
    outs, sems = refs[:-1], refs[-1]
    copies = []
    for i, out in enumerate(outs):
        start = pl.multiple_of(place_ref[i] * LANES, LANES)
        rows = w_ref.at[pl.ds(start, out.shape[0]), :]
        copies.append(pltpu.make_async_copy(rows, out, sems.at[i]))
    for copy in copies:
        copy.start()
    for copy in copies:
        copy.wait()


def cut(w_out, rows, places):
    return pl.pallas_call(
        cut_body,
        in_specs=[TABLE, STAY],
        out_specs=[WHOLE] * len(places),
        out_shape=[jax.ShapeDtypeStruct((rows, w_out.shape[1]), w_out.dtype)] * len(places),
        scratch_shapes=[pltpu.SemaphoreType.DMA((len(places),))],
        compiler_params=params(),
        name="cut",
    )(jnp.stack(places), far_memory(w_out))


def project_body(count, place_ref, far_ref, near_ref, *refs):
    for act_ref, out_ref in zip((far_ref, near_ref), refs[-2:]):
        total = None
        for i, chunk in enumerate(refs[:count]):
            if count == 1:
                part = act_ref[...]
            else:
                start = pl.multiple_of(place_ref[i] * LANES, LANES)
                part = act_ref[:, pl.ds(start, chunk.shape[0])]
            term = jnp.dot(part, chunk[...], preferred_element_type=jnp.float32)
            total = term if total is None else total + term
        out_ref[...] = total.astype(jnp.bfloat16)


def project(far, near, chunks, places, shard, columns, out):
    tokens, channels = near.shape
    width = chunks[0].shape[1]
    block = min(width, 256)
    steps = width // block
    act_spec = pl.BlockSpec((tokens, channels), lambda i, place: (0, 0))
    in_specs = [act_spec] * 2
    in_specs += [pl.BlockSpec((chunk.shape[0], block), lambda i, place: (0, i)) for chunk in chunks]
    operands = [far, near, *chunks]
    aliases = {}
    if out is not None:
        aliases = {len(operands) + 1: 1}
        in_specs.append(STAY)
        operands.append(out)
    flops = 4 * tokens * channels * width
    return pl.pallas_call(
        functools.partial(project_body, len(chunks)),
        grid_spec=pltpu.PrefetchScalarGridSpec(
            num_scalar_prefetch=1,
            grid=(steps,),
            in_specs=in_specs,
            out_specs=[
                pl.BlockSpec((tokens, block), lambda i, place: (0, i)),
                pl.BlockSpec(
                    (tokens, block), lambda i, place: (0, place[len(places)] * steps + i)
                ),
            ],
        ),
        out_shape=[
            jax.ShapeDtypeStruct((tokens, width), jnp.bfloat16),
            pltpu.HBM((tokens, columns), jnp.bfloat16),
        ],
        input_output_aliases=aliases,
        compiler_params=pltpu.CompilerParams(
            dimension_semantics=("arbitrary",), vmem_limit_bytes=16 << 20
        ),
        cost_estimate=cost(flops, 2 * channels * (2 * tokens + width)),
        name="project",
    )(jnp.stack([*places, shard]), *operands)


def collect_body(place_ref, *refs):
    pieces, out_ref, sems = refs[:-3], refs[-2], refs[-1]
    width = pieces[0].shape[1]
    copies = []
    for i, piece in enumerate(pieces):
        at = pl.multiple_of(place_ref[i] * width, LANES)
        copies.append(pltpu.make_async_copy(piece, out_ref.at[:, pl.ds(at, width)], sems.at[i]))
    for copy in copies:
        copy.start()
    for copy in copies:
        copy.wait()


def collect(pieces, shards, out):
    return pl.pallas_call(
        collect_body,
        in_specs=[TABLE] + [WHOLE] * len(pieces) + [STAY],
        out_specs=STAY,
        out_shape=jax.ShapeDtypeStruct(out.shape, out.dtype),
        scratch_shapes=[pltpu.SemaphoreType.DMA((len(pieces),))],
        input_output_aliases={1 + len(pieces): 0},
        compiler_params=params(),
        name="collect",
    )(jnp.stack(shards), *pieces, out)


def per_device(lin_pre, gate_pre, w_depth, ln_gain, ln_shift, w_out):
    dp, sp = lax.axis_size("dp"), lax.axis_size("sp")
    chips = dp // 2
    mine, place = lax.axis_index("dp"), lax.axis_index("sp")
    spot = place % 4
    parity = (place % 2)[None]
    tiles = w_out.shape[0] // 4 // LANES

    def to_sibling(x):
        return lax.ppermute(x, "dp", [(i, i ^ 1) for i in range(dp)])

    def to_near(x, bit):
        return lax.ppermute(x, "sp", [(i, i ^ bit) for i in range(sp)])

    places = [unit * tiles for unit in (spot, 3 - spot, spot ^ 1, spot ^ 2)]
    first, second = cut(w_out, w_out.shape[0] // 4, places[:2])
    hops = [
        [(i, (i // 2 + k) % chips * 2 + i % 2) for i in range(dp)] for k in range(1, chips)
    ]
    direct_a = [lax.ppermute(first, "dp", perm) for perm in hops]
    direct_b = [lax.ppermute(second, "dp", perm) for perm in hops]

    glu, to_pair, to_next = gated(parity, far_memory(lin_pre), far_memory(gate_pre))
    odd = [(i, i + 1) for i in range(1, sp - 1, 2)]
    from_pair = to_near(to_pair, 1)
    from_next = lax.ppermute(to_next, "sp", odd + [(j, i) for i, j in odd])
    gain, shift = ln_gain[None, :], ln_shift[None, :]
    act = activated_inner(glu, w_depth, gain, shift)
    direct_a, act = lax.optimization_barrier((direct_a, act))
    by_x = [to_near(part, 1) for part in direct_a]
    by_z = [to_near(part, 2) for part in direct_a]
    from_pair, from_next, act = lax.optimization_barrier((from_pair, from_next, act))
    act = activated_outer(parity, from_pair, from_next, glu, w_depth, gain, shift, act)

    act_far = to_sibling(act)
    columns = w_out.shape[1] * dp
    own_far, out = project(act_far, act, [far_memory(w_out)], places[:1], mine, columns, None)
    shards = [mine ^ 1]
    received = [to_sibling(own_far)]
    for k in range(1, chips):
        chunks = [arrival[k - 1] for arrival in (direct_a, direct_b, by_x, by_z)]
        source = (mine // 2 - k) % chips * 2 + mine % 2
        other_far, out = project(act_far, act, chunks, places, source, columns, out)
        received.append(to_sibling(other_far))
        shards.append(source ^ 1)
    return collect(received, shards, out)


def solution(mesh):
    in_specs = (P(None, ("dp", "sp")), P(None, ("dp", "sp")), P(), P(), P(), P(None, "dp"))
    out_specs = P(("dp", "sp"), None)
    return jax.shard_map(
        per_device, mesh=mesh, in_specs=in_specs, out_specs=out_specs, check_vma=False
    )
```

```python
import functools

import jax
import jax.numpy as jnp
from jax import lax
from jax.experimental import pallas as pl
from jax.experimental.pallas import tpu as pltpu
from jax.sharding import PartitionSpec as P


LANES = 128
EDGE = 16
EPS = 1e-05
WHOLE = pl.BlockSpec(memory_space=pltpu.VMEM)
STAY = pl.BlockSpec(memory_space=pltpu.HBM)
TABLE = pl.BlockSpec(memory_space=pltpu.SMEM)


def params(semantics=None):
    return pltpu.CompilerParams(dimension_semantics=semantics, vmem_limit_bytes=16 << 20)


def cost(flops, nbytes):
    return pl.CostEstimate(flops=flops, transcendentals=0, bytes_accessed=nbytes)


def glu_body(parity_ref, lin_ref, gate_ref, out_ref, near_ref, next_ref):
    gate = gate_ref[...].astype(jnp.float32)
    glu = (lin_ref[...].astype(jnp.float32) * jax.nn.sigmoid(gate)).T.astype(jnp.bfloat16)
    out_ref[...] = glu
    head, tail = glu[:EDGE], glu[glu.shape[0] - EDGE :]
    even = parity_ref[0] == 0
    near_ref[...] = jnp.where(even, tail, head)
    next_ref[...] = jnp.where(even, head, tail)


def gated(parity, lin_pre, gate_pre):
    channels, tokens = lin_pre.shape
    block = 256
    edge = pl.BlockSpec((EDGE, block), lambda i: (0, i))
    return pl.pallas_call(
        glu_body,
        grid=(channels // block,),
        in_specs=[TABLE] + [pl.BlockSpec((block, tokens), lambda i: (i, 0))] * 2,
        out_specs=[pl.BlockSpec((tokens, block), lambda i: (0, i)), edge, edge],
        out_shape=[
            jax.ShapeDtypeStruct((tokens, channels), jnp.bfloat16),
            jax.ShapeDtypeStruct((EDGE, channels), jnp.bfloat16),
            jax.ShapeDtypeStruct((EDGE, channels), jnp.bfloat16),
        ],
        compiler_params=params(("arbitrary",)),
        cost_estimate=cost(20 * channels * tokens, 6 * channels * tokens),
        name="glu",
    )(parity, lin_pre, gate_pre)


def conv_norm(cells, w_ref, gain_ref, shift_ref, mixed, start, tiles, store):
    blocks = cells.shape[0]
    span = 8 * tiles
    channels = blocks * LANES
    taps = w_ref.shape[0]

    def one_block(block, total):
        lanes = pl.ds(pl.multiple_of(block * LANES, LANES), LANES)
        running = [jnp.zeros((span, LANES), jnp.float32) for _ in range(2)]
        turn = 0
        lead = EDGE - (taps - 1) // 2
        for phase in range(8):
            window = cells[block, pl.ds(start - EDGE + phase, span + 8 * 3), :]
            for whole in range(4):
                tap = 8 * whole + phase - lead
                if 0 <= tap < taps:
                    weight = w_ref[pl.ds(tap, 1), lanes]
                    running[turn] = running[turn] + weight * window[8 * whole : 8 * whole + span]
                    turn = 1 - turn
        value = (running[0] + running[1]).astype(jnp.bfloat16).astype(jnp.float32)
        mixed[block, pl.ds(0, span), :] = value
        return total + value

    zeros = jnp.zeros((span, LANES), jnp.float32)
    total = lax.fori_loop(0, blocks, one_block, zeros)
    mean = jnp.broadcast_to(jnp.sum(total, axis=1, keepdims=True) / channels, (span, LANES))

    square = zeros
    for block in range(blocks):
        square = square + jnp.square(mixed[block, pl.ds(0, span), :] - mean)
    variance = jnp.sum(square, axis=1, keepdims=True) / channels
    scale = jnp.broadcast_to(lax.rsqrt(variance + EPS), (span, LANES))
    for block in range(blocks):
        lanes = pl.ds(block * LANES, LANES)
        normed = (mixed[block, pl.ds(0, span), :] - mean) * scale
        normed = normed * gain_ref[:, lanes] + shift_ref[:, lanes]
        store(lanes, (normed * jax.nn.sigmoid(normed)).astype(jnp.bfloat16))


def inner_body(tiles, glu_ref, w_ref, gain_ref, shift_ref, out_ref, cells, mixed):
    blocks = cells.shape[0]
    for block in range(blocks):
        cells[block] = glu_ref[:, pl.ds(block * LANES, LANES)].astype(jnp.float32)
    span = 8 * tiles

    def chunk(i, carry):
        start = pl.multiple_of(EDGE + i * span, 8)

        def store(lanes, value):
            out_ref[pl.ds(start, span), lanes] = value

        conv_norm(cells, w_ref, gain_ref, shift_ref, mixed, start, tiles, store)
        return carry

    lax.fori_loop(0, (glu_ref.shape[0] - 2 * EDGE) // span, chunk, 0)


def outer_body(parity_ref, near_ref, next_ref, glu_ref, w_ref, gain_ref, shift_ref, _, out_ref, cells, mixed):
    side = pl.program_id(0)
    blocks = cells.shape[0]
    for block in range(blocks):
        lanes = pl.ds(block * LANES, LANES)
        own = glu_ref[:, lanes].astype(jnp.float32)
        halo = jnp.where(side != parity_ref[0], near_ref[:, lanes], next_ref[:, lanes])
        halo = halo.astype(jnp.float32)
        cells[block, pl.ds(EDGE, 2 * EDGE), :] = jnp.where(side == 0, own, 0.0)
        cells[block, pl.ds(0, EDGE), :] = jnp.where(side == 0, halo, own[:EDGE])
        cells[block, pl.ds(EDGE, EDGE), :] = jnp.where(side == 0, own[:EDGE], own[EDGE:])
        cells[block, pl.ds(2 * EDGE, EDGE), :] = jnp.where(side == 0, own[EDGE:], halo)

    def store(lanes, value):
        out_ref[:, lanes] = value

    conv_norm(cells, w_ref, gain_ref, shift_ref, mixed, EDGE, EDGE // 8, store)


def activated_inner(glu, w_depth, gain, shift):
    tokens, channels = glu.shape
    inner = (tokens - 2 * EDGE) // 16
    tiles = 2 * max(n for n in range(1, 5) if inner % n == 0)
    blocks = channels // LANES
    return pl.pallas_call(
        functools.partial(inner_body, tiles),
        out_shape=jax.ShapeDtypeStruct((tokens, channels), jnp.bfloat16),
        scratch_shapes=[
            pltpu.VMEM((blocks, tokens, LANES), jnp.float32),
            pltpu.VMEM((blocks, 8 * tiles, LANES), jnp.float32),
        ],
        compiler_params=params(),
        cost_estimate=cost(80 * channels * tokens, 4 * channels * tokens),
        name="conv_inner",
    )(glu, w_depth, gain, shift)


def activated_outer(parity, near, ahead, glu, w_depth, gain, shift, act):
    tokens, channels = glu.shape
    blocks = channels // LANES
    whole = pl.BlockSpec((EDGE, channels), lambda i: (0, 0))
    row = pl.BlockSpec((1, channels), lambda i: (0, 0))
    last = tokens // EDGE - 1
    return pl.pallas_call(
        outer_body,
        grid=(2,),
        in_specs=[
            TABLE,
            whole,
            whole,
            pl.BlockSpec((2 * EDGE, channels), lambda i: (i * (tokens // (2 * EDGE) - 1), 0)),
            pl.BlockSpec(w_depth.shape, lambda i: (0, 0)),
            row,
            row,
            pl.BlockSpec(memory_space=pl.ANY),
        ],
        out_specs=pl.BlockSpec((EDGE, channels), lambda i: (i * last, 0)),
        out_shape=jax.ShapeDtypeStruct((tokens, channels), jnp.bfloat16),
        scratch_shapes=[
            pltpu.VMEM((blocks, 3 * EDGE, LANES), jnp.float32),
            pltpu.VMEM((blocks, EDGE, LANES), jnp.float32),
        ],
        input_output_aliases={7: 0},
        compiler_params=params(("arbitrary",)),
        cost_estimate=cost(80 * channels * 2 * EDGE, 8 * channels * EDGE),
        name="conv_outer",
    )(parity, near, ahead, glu, w_depth, gain, shift, act)


def quarters_body(place_ref, w_ref, *refs):
    outs, sems = refs[:-1], refs[-1]
    rows = outs[0].shape[0]
    copies = [
        pltpu.make_async_copy(w_ref.at[pl.ds(place_ref[i] * rows, rows), :], out, sems.at[i])
        for i, out in enumerate(outs)
    ]
    for copy in copies:
        copy.start()
    for copy in copies:
        copy.wait()


def quarters(w_out, units):
    shape = jax.ShapeDtypeStruct((w_out.shape[0] // 4, w_out.shape[1]), w_out.dtype)
    return pl.pallas_call(
        quarters_body,
        in_specs=[TABLE, STAY],
        out_specs=[WHOLE] * len(units),
        out_shape=[shape] * len(units),
        scratch_shapes=[pltpu.SemaphoreType.DMA((len(units),))],
        compiler_params=params(),
        name="quarters",
    )(jnp.stack(units), pltpu.with_memory_space_constraint(w_out, pltpu.HBM))


def project_body(place_ref, act_ref, *refs):
    chunks, out_ref = refs[:-1], refs[-1]
    rows = chunks[0].shape[0]
    total = None
    for i, chunk in enumerate(chunks):
        if len(chunks) == 1:
            part = act_ref[...]
        else:
            part = act_ref[:, pl.ds(pl.multiple_of(place_ref[i] * rows, LANES), rows)]
        term = jnp.dot(part, chunk[...], preferred_element_type=jnp.float32)
        total = term if total is None else total + term
    out_ref[...] = total.astype(jnp.bfloat16)


def project(act, chunks, units):
    tokens, channels = act.shape
    width = chunks[0].shape[1]
    return pl.pallas_call(
        project_body,
        in_specs=[TABLE] + [WHOLE] * (1 + len(chunks)),
        out_specs=WHOLE,
        out_shape=jax.ShapeDtypeStruct((tokens, width), jnp.bfloat16),
        compiler_params=params(),
        cost_estimate=cost(2 * tokens * channels * width, 2 * channels * (tokens + width)),
        name="project",
    )(jnp.stack(units), act, *chunks)


def collect_body(place_ref, *refs):
    pieces, out_ref, sems = refs[:-2], refs[-2], refs[-1]
    width = pieces[0].shape[1]
    copies = []
    for i, piece in enumerate(pieces):
        at = pl.multiple_of(place_ref[i] * width, LANES)
        copies.append(pltpu.make_async_copy(piece, out_ref.at[:, pl.ds(at, width)], sems.at[i]))
    for copy in copies:
        copy.start()
    for copy in copies:
        copy.wait()


def collect(pieces, shards):
    tokens, width = pieces[0].shape
    return pl.pallas_call(
        collect_body,
        in_specs=[TABLE] + [WHOLE] * len(pieces),
        out_specs=STAY,
        out_shape=jax.ShapeDtypeStruct((tokens, width * len(pieces)), jnp.bfloat16),
        scratch_shapes=[pltpu.SemaphoreType.DMA((len(pieces),))],
        compiler_params=params(),
        name="collect",
    )(jnp.stack(shards), *pieces)


def per_device(lin_pre, gate_pre, w_depth, ln_gain, ln_shift, w_out):
    dp, sp = lax.axis_size("dp"), lax.axis_size("sp")
    chips = dp // 2
    mine = lax.axis_index("dp")
    spot = lax.axis_index("sp") % 4
    parity = (lax.axis_index("sp") % 2)[None]

    def to_sibling(x):
        return lax.ppermute(x, "dp", [(i, i ^ 1) for i in range(dp)])

    def to_near(x, bit):
        return lax.ppermute(x, "sp", [(i, i ^ bit) for i in range(sp)])

    (first,) = quarters(w_out, (spot,))
    (second,) = quarters(w_out, (3 - spot,))
    hops = [
        [(i, (i // 2 + k) % chips * 2 + i % 2) for i in range(dp)] for k in range(1, chips)
    ]
    direct_a = [lax.ppermute(first, "dp", perm) for perm in hops]
    direct_b = [lax.ppermute(second, "dp", perm) for perm in hops]

    glu, to_pair, to_next = gated(parity, lin_pre, gate_pre)
    odd = [(i, i + 1) for i in range(1, sp - 1, 2)]
    from_pair = to_near(to_pair, 1)
    from_next = lax.ppermute(to_next, "sp", odd + [(j, i) for i, j in odd])
    gain, shift = ln_gain[None, :], ln_shift[None, :]
    act = activated_inner(glu, w_depth, gain, shift)
    direct_a, act = lax.optimization_barrier((direct_a, act))
    by_x = [to_near(a, 1) for a in direct_a]
    by_z = [to_near(a, 2) for a in direct_a]
    from_pair, from_next, act = lax.optimization_barrier((from_pair, from_next, act))
    act = activated_outer(parity, from_pair, from_next, glu, w_depth, gain, shift, act)

    act_far = to_sibling(act)
    pieces, shards = [project(act, [w_out], (spot,))], [mine]
    own_far = project(act_far, [w_out], (spot,))
    received = [to_sibling(own_far)]
    by_x, by_z, direct_b, act_far, act, pieces = lax.optimization_barrier(
        (by_x, by_z, direct_b, act_far, act, pieces)
    )
    units = (spot, 3 - spot, spot ^ 1, spot ^ 2)
    for k in range(1, chips):
        near = [direct_a[k - 1], direct_b[k - 1], by_x[k - 1], by_z[k - 1]]
        other_far = project(act_far, near, units)
        received.append(to_sibling(other_far))
        pieces.append(project(act, near, units))
        shards.append((mine // 2 - k) % chips * 2 + mine % 2)
    return collect(pieces + received, shards + [shard ^ 1 for shard in shards])


def solution(mesh):
    in_specs = (P(None, ("dp", "sp")), P(None, ("dp", "sp")), P(), P(), P(), P(None, "dp"))
    out_specs = P(("dp", "sp"), None)
    return jax.shard_map(
        per_device, mesh=mesh, in_specs=in_specs, out_specs=out_specs, check_vma=False
    )
```
